32 devices in a mesh: sp: 4 (over z), dp: 8 (over y, x, core).
Axes of the slice: x: 2, y: 2, z: 4, core: 2. Of those that a mesh axis runs over, the one named last changes fastest.
Arguments:
- hidden_states: bfloat16 [8, 512, 2048], P('dp', 'sp'), may hold values from -6 to 6
- queries: bfloat16 [8, 512, 2048], P('dp', 'sp'), may hold values from -12 to 12
- key_shift: bfloat16 [8, 512, 16], P('dp', 'sp'), may hold values from -15 to 0
- key_weight: bfloat16 [2048, 256], P('dp'), may hold values from -0.125 to 0.125
- value_weight: bfloat16 [2048, 256], P('dp'), may hold values from -0.125 to 0.125
Outputs:
- attended: bfloat16 [8, 512, 2048], P('dp', 'sp')
The draws below stay inside these ranges and needn't reach their ends.
All inputs are finite; a program needn't handle non-finite values.
Results may differ from the reference program's by a relative error of at most 0.0079.
Values may be sent and summed in bfloat16 or wider, within the bound.
A program may use at most 64 MiB of HBM per device.

```python
import jax
import jax.numpy as jnp
from jax import lax

D = 2048
QUERY_HEAD_COUNT = 16
KV_HEADS = 2
HEAD_DIM = 128
TOK_DEV = 128
SEQUENCE_COUNT = 8
SEQUENCE_LENGTH = 512


def draw_key_shift(key, part):
    base_key = jax.random.fold_in(key, 11)
    coin_key, slow_key, fast_key, block_key, rough_key, location_random_key, level_random_key = jax.random.split(base_key, 7)
    coin_flip = jax.random.randint(coin_key, (QUERY_HEAD_COUNT,), 0, 2)
    slow_base = jax.random.uniform(slow_key, (QUERY_HEAD_COUNT,), jnp.float32, -13.0, -11.5)
    fast_base = jax.random.uniform(fast_key, (QUERY_HEAD_COUNT,), jnp.float32, -9.0, -8.0)
    head_offset = jnp.where(coin_flip == 1, fast_base, slow_base)
    block_count = SEQUENCE_LENGTH // TOK_DEV
    block_slope = jax.random.uniform(block_key, (SEQUENCE_COUNT, block_count, 1, QUERY_HEAD_COUNT), jnp.float32, -0.7, 0.7)
    block_slope = jnp.broadcast_to(block_slope, (SEQUENCE_COUNT, block_count, TOK_DEV, QUERY_HEAD_COUNT)).reshape(SEQUENCE_COUNT, SEQUENCE_LENGTH, QUERY_HEAD_COUNT)
    noise_amplitude = jax.random.uniform(rough_key, (SEQUENCE_COUNT, SEQUENCE_LENGTH, QUERY_HEAD_COUNT), jnp.float32, -0.5, 0.5)
    spike_locations = jax.random.randint(location_random_key, (SEQUENCE_COUNT, 4), 0, SEQUENCE_LENGTH)
    position_indices = jnp.arange(SEQUENCE_LENGTH, dtype=jnp.int32)
    spike_mask = jnp.any(position_indices[None, :, None] == spike_locations[:, None, :], axis=2)
    spike_level = jax.random.uniform(level_random_key, (SEQUENCE_COUNT, SEQUENCE_LENGTH, QUERY_HEAD_COUNT), jnp.float32, -1.5, 0.0)
    shifted_values = jnp.where(spike_mask[:, :, None], spike_level, head_offset[None, None, :] + block_slope + noise_amplitude)
    return shifted_values.astype(jnp.bfloat16)


def block_scale(own_key, dims, shards, smallest, high):
    loudness = 1.0
    for dim, parts in shards:
        steps = jax.random.uniform(jax.random.fold_in(jax.random.fold_in(own_key, 6), dim), (parts,), jnp.float32, smallest / len(shards), high / len(shards))
        loudness = loudness * jnp.repeat(jnp.exp(steps), dims[dim] // parts).reshape((-1,) + (1,) * (len(dims) - 1 - dim))
    return loudness


def scatter_about(stream_key, dims, width, limit, cuts=(), kind=jnp.bfloat16):
    entries = jax.random.normal(stream_key, dims, jnp.float32) * width
    if len(cuts) > 0:
        entries = block_scale(stream_key, dims, cuts, -0.22, 0.18) * entries
    return jnp.clip(entries, min=-limit, max=limit).astype(kind)


def setup_inputs(seed: int = 0) -> dict:
    keys = jax.random.split(jax.random.key(seed), 6)
    hidden_states = scatter_about(keys[0], (SEQUENCE_COUNT, SEQUENCE_LENGTH, D), 1.0, 6.0, ((0, 8), (1, 4)))
    queries = scatter_about(keys[1], (SEQUENCE_COUNT, SEQUENCE_LENGTH, QUERY_HEAD_COUNT * HEAD_DIM), 3.0, 12.0, ((0, 8), (1, 4)))
    key_shift = draw_key_shift(jax.random.fold_in(keys[5], 71), 0)
    key_weight = scatter_about(keys[3], (D, KV_HEADS * HEAD_DIM), D ** -0.5, 0.125, ((0, 8),))
    value_weight = scatter_about(keys[4], (D, KV_HEADS * HEAD_DIM), D ** -0.5, 0.125, ((0, 8),))
    return {"hidden_states": hidden_states, "queries": queries, "key_shift": key_shift, "key_weight": key_weight, "value_weight": value_weight}


def reference(hidden_states, queries, key_shift, key_weight, value_weight):
    seq_len = hidden_states.shape[1]
    group_size = QUERY_HEAD_COUNT // KV_HEADS
    block_len = min(512, seq_len)
    position_indices = jnp.arange(seq_len, dtype=jnp.int32)

    def one_sequence(inputs):
        token_rows, query_rows, shift_rows = inputs
        key_rows = jnp.dot(token_rows, key_weight, preferred_element_type=jnp.float32).astype(jnp.bfloat16)
        value_rows = jnp.dot(token_rows, value_weight, preferred_element_type=jnp.float32).astype(jnp.bfloat16)
        query_float = query_rows.reshape(seq_len, QUERY_HEAD_COUNT, HEAD_DIM).astype(jnp.float32)
        key_float = jnp.repeat(key_rows.reshape(seq_len, KV_HEADS, HEAD_DIM).astype(jnp.float32), group_size, axis=1)
        value_float = jnp.repeat(value_rows.reshape(seq_len, KV_HEADS, HEAD_DIM).astype(jnp.float32), group_size, axis=1)
        shift_float = shift_rows.astype(jnp.float32)
        pieces = []
        for block_index in range(seq_len // block_len):
            first_row = block_index * block_len
            last_row = first_row + block_len
            logits = jnp.einsum("qhd,khd->hqk", query_float[first_row:last_row], key_float[:last_row])
            logits = logits * (HEAD_DIM ** -0.5) + shift_float[:last_row].T[:, None, :]
            visible = position_indices[None, :last_row] < position_indices[first_row:last_row, None]
            penalty = jnp.where(visible, jax.nn.softplus(logits), 0.0)
            suffix_sum = lax.cumsum(penalty, axis=2, reverse=True) - penalty
            weights = jnp.where(visible, jnp.exp(jax.nn.log_sigmoid(logits) - suffix_sum), 0.0)
            weights = lax.optimization_barrier(weights.astype(jnp.bfloat16)).astype(jnp.float32)
            mixed_rows = jnp.einsum("hqk,khd->qhd", weights, value_float[:last_row])
            pieces.append(mixed_rows.reshape(block_len, QUERY_HEAD_COUNT * HEAD_DIM))
        return jnp.concatenate(pieces, axis=0).astype(jnp.bfloat16)

    return lax.map(one_sequence, (hidden_states, queries, key_shift))
```

```python
import functools
import math

import jax
import jax.numpy as jnp
from jax import lax
from jax.experimental import pallas as pl
from jax.experimental.pallas import tpu as pltpu
from jax.sharding import PartitionSpec as P

HEAD_DIM = 128
LOG2E = math.log2(math.e)
MESH = pl.DeviceIdType.MESH
NT = (((1,), (1,)), ((), ()))


def chip_peers(chip, chips):
    if chips == 4:
        x, y = chip % 2, chip // 2
        order = [chip + 1 - 2 * x, chip + 2 - 4 * y, chips - 1 - chip]
        return [(c, c) for c in order]
    return [((chip + k) % chips, (chip + chips - k) % chips) for k in range(1, chips)]


def kernel(
    n_sp, n_dp,
    x_hbm, q_hbm, sh_hbm, wk_hbm, wv_hbm, out_ref,
    x, q, sh, w_all, kv, sh_all, wts, acc, carried, tri,
    load_sem, ici_send, ici_recv, d2d_send, d2d_recv, z_send, z_recv,
):
    s, d = lax.axis_index("sp"), lax.axis_index("dp")
    chips = n_dp // 2
    chip, core = d // 2, d % 2
    partner = d + 1 - 2 * core
    peers = chip_peers(chip, chips)
    tok, model = x.shape
    heads = sh.shape[1]
    groups = kv.shape[3] // HEAD_DIM
    per_group = heads // groups

    loads = [
        pltpu.make_async_copy(wk_hbm, w_all.at[0, d], load_sem.at[0]),
        pltpu.make_async_copy(wv_hbm, w_all.at[1, d], load_sem.at[1]),
        pltpu.make_async_copy(sh_hbm, sh, load_sem.at[2]),
        pltpu.make_async_copy(x_hbm, x, load_sem.at[3]),
        pltpu.make_async_copy(q_hbm, q, load_sem.at[4]),
    ]
    for load in loads:
        load.start()

    barrier = pltpu.get_barrier_semaphore()
    for to, _ in peers:
        pl.semaphore_signal(barrier, inc=1, device_id={"dp": to * 2 + core}, device_id_type=MESH)
    pl.semaphore_signal(barrier, inc=1, device_id={"dp": partner}, device_id_type=MESH)
    for t in range(1, n_sp):
        pl.semaphore_signal(barrier, inc=1, device_id={"sp": (s + t) % n_sp}, device_id_type=MESH)
    pl.semaphore_wait(barrier, chips - 1 + 1 + n_sp - 1)

    def ici_copy(part, k, block, to):
        return pltpu.make_async_remote_copy(
            src_ref=w_all.at[part, block], dst_ref=w_all.at[part, block],
            send_sem=ici_send.at[part, k], recv_sem=ici_recv.at[part, k],
            device_id={"dp": to * 2 + core}, device_id_type=MESH)

    def d2d_copy(part, k, block):
        return pltpu.make_async_remote_copy(
            src_ref=w_all.at[part, block], dst_ref=w_all.at[part, block],
            send_sem=d2d_send.at[part, k], recv_sem=d2d_recv.at[part, k],
            device_id={"dp": partner}, device_id_type=MESH)

    def z_copy(part, t, block, to):
        ref = sh_all.at[block] if part == 2 else kv.at[part, block]
        return pltpu.make_async_remote_copy(
            src_ref=ref, dst_ref=ref,
            send_sem=z_send.at[part, t], recv_sem=z_recv.at[part, t],
            device_id={"sp": to}, device_id_type=MESH)

    for part in range(2):
        loads[part].wait()
        for k, (to, _) in enumerate(peers, 1):
            ici_copy(part, k, d, to).start()
        d2d_copy(part, 0, d).start()

    loads[2].wait()
    eye = (
        lax.broadcasted_iota(jnp.int32, (heads, heads), 0)
        == lax.broadcasted_iota(jnp.int32, (heads, heads), 1)
    ).astype(jnp.bfloat16)
    sh_all[s] = lax.dot_general(eye, sh[...], NT, preferred_element_type=jnp.float32).astype(jnp.bfloat16)
    row = lax.broadcasted_iota(jnp.int32, tri.shape, 0)
    col = lax.broadcasted_iota(jnp.int32, tri.shape, 1)
    tri[...] = ((row > col) | (col >= tok)).astype(jnp.bfloat16)

    def send_up(part):
        for t in range(1, n_sp):
            @pl.when(s + t < n_sp)
            def _(t=t):
                z_copy(part, t, s, s + t).start()

    send_up(2)

    def gather(part):
        for k, (_, source) in enumerate(peers, 1):
            block = source * 2 + core
            ici_copy(part, k, block, chip).wait_recv()
            d2d_copy(part, k, block).start()
        d2d_copy(part, 0, partner).wait_recv()
        for k, (_, source) in enumerate(peers, 1):
            d2d_copy(part, k, source * 2 + 1 - core).wait_recv()

    def project(part):
        weight = w_all[part].reshape(model, w_all.shape[3])
        kv[part, s] = jnp.dot(x[...], weight, preferred_element_type=jnp.float32).astype(jnp.bfloat16)

    def weigh(block, diagonal):
        keys = kv[0, block]
        shift = sh_all[block].astype(jnp.float32) * LOG2E
        scale = HEAD_DIM ** -0.5 * LOG2E
        if diagonal:
            visible = lax.broadcasted_iota(jnp.int32, (tok, tok), 1) < lax.broadcasted_iota(
                jnp.int32, (tok, tok), 0)
        for h in range(heads):
            g = h // per_group
            z = lax.dot_general(
                q[:, h * HEAD_DIM:(h + 1) * HEAD_DIM], keys[:, g * HEAD_DIM:(g + 1) * HEAD_DIM], NT,
                preferred_element_type=jnp.float32)
            z = z * scale + shift[h:h + 1, :]
            p = jnp.maximum(z, jnp.log(1.0 + jnp.exp2(jnp.minimum(z, 100.0))) * LOG2E)
            if diagonal:
                p = jnp.where(visible, p, 0.0)
            sums = jnp.dot(p.astype(jnp.bfloat16), tri[...], preferred_element_type=jnp.float32)
            power = z - p - sums[:, :tok]
            total = sums[:, tok:]
            if diagonal:
                w = jnp.where(visible, jnp.exp2(power), 0.0)
                carried[h] = total
            else:
                before = carried[h]
                w = jnp.exp2(power - before)
                carried[h] = before + total
            wts[block, h] = w.astype(jnp.bfloat16)

    def mix(block, first):
        values = kv[1, block]
        for g in range(groups):
            span = slice(g * per_group, (g + 1) * per_group)
            w = wts[block, span].reshape(per_group * tok, tok)
            term = jnp.dot(w, values[:, g * HEAD_DIM:(g + 1) * HEAD_DIM], preferred_element_type=jnp.float32)
            term = term.reshape(per_group, tok, HEAD_DIM)
            acc[span] = term if first else acc[span] + term

    gather(0)
    loads[3].wait()
    project(0)
    send_up(0)
    loads[4].wait()
    weigh(s, True)
    gather(1)
    project(1)
    send_up(1)

    @pl.loop(1, s + 1)
    def _(t):
        z_copy(2, t, s - t, s).wait_recv()
        z_copy(0, t, s - t, s).wait_recv()
        weigh(s - t, False)

    mix(s, True)

    @pl.loop(1, s + 1)
    def _(t):
        z_copy(1, t, s - t, s).wait_recv()
        mix(s - t, False)

    for h in range(heads):
        out_ref[:, h * HEAD_DIM:(h + 1) * HEAD_DIM] = acc[h].astype(out_ref.dtype)

    for part in range(2):
        for k, (to, source) in enumerate(peers, 1):
            ici_copy(part, k, d, to).wait_send()
            d2d_copy(part, k, source * 2 + core).wait_send()
        d2d_copy(part, 0, d).wait_send()
    for part in range(3):
        for t in range(1, n_sp):
            @pl.when(s + t < n_sp)
            def _(part=part, t=t):
                z_copy(part, t, s, s + t).wait_send()


def per_device(n_sp, n_dp, hidden_states, queries, key_shift, key_weight, value_weight):
    seq_local, tok, model = hidden_states.shape
    assert seq_local == 1
    width, heads = queries.shape[2], key_shift.shape[2]
    rows, kv_width = key_weight.shape
    chips = n_dp // 2
    bf16, f32 = jnp.bfloat16, jnp.float32
    dma = pltpu.SemaphoreType.DMA
    out = pl.pallas_call(
        functools.partial(kernel, n_sp, n_dp),
        out_shape=jax.ShapeDtypeStruct((tok, width), bf16),
        in_specs=[pl.BlockSpec(memory_space=pl.ANY)] * 5,
        out_specs=pl.BlockSpec(memory_space=pltpu.VMEM),
        scratch_shapes=[
            pltpu.VMEM((tok, model), bf16),
            pltpu.VMEM((tok, width), bf16),
            pltpu.VMEM((tok, heads), bf16),
            pltpu.VMEM((2, n_dp, rows, kv_width), bf16),
            pltpu.VMEM((2, n_sp, tok, kv_width), bf16),
            pltpu.VMEM((n_sp, heads, tok), bf16),
            pltpu.VMEM((n_sp, heads, tok, tok), bf16),
            pltpu.VMEM((heads, tok, HEAD_DIM), f32),
            pltpu.VMEM((heads, tok, tok), f32),
            pltpu.VMEM((tok, 2 * tok), bf16),
            dma((5,)),
            dma((2, chips)), dma((2, chips)),
            dma((2, chips)), dma((2, chips)),
            dma((3, n_sp)), dma((3, n_sp)),
        ],
        compiler_params=pltpu.CompilerParams(collective_id=0, has_side_effects=True),
        name="stick_breaking",
    )(hidden_states[0], queries[0], key_shift[0], key_weight, value_weight)
    return out[None]


def solution(mesh):
    placed = (
        P("dp", "sp", None),
        P("dp", "sp", None),
        P("dp", "sp", None),
        P("dp", None),
        P("dp", None),
    )
    return jax.shard_map(
        functools.partial(per_device, mesh.shape["sp"], mesh.shape["dp"]),
        mesh=mesh, in_specs=placed, out_specs=P("dp", "sp", None), check_vma=False,
    )
```

```python
import functools
import math

import jax
import jax.numpy as jnp
from jax import lax
from jax.experimental import pallas as pl
from jax.experimental.pallas import tpu as pltpu
from jax.sharding import PartitionSpec as P

HEAD_DIM = 128
LOG2E = math.log2(math.e)
MESH = pl.DeviceIdType.MESH
NT = (((1,), (1,)), ((), ()))


def chip_peers(chip, chips):
    if chips == 4:
        x, y = chip % 2, chip // 2
        order = [chip + 1 - 2 * x, chip + 2 - 4 * y, chips - 1 - chip]
        return [(c, c) for c in order]
    return [((chip + k) % chips, (chip + chips - k) % chips) for k in range(1, chips)]


def kernel(
    n_sp, n_dp,
    x_hbm, q_hbm, sh_hbm, wk_hbm, wv_hbm, out_ref,
    x, q, w_all, kv, sh_all, wts, acc, carried, tri,
    load_sem, ici_send, ici_recv, d2d_send, d2d_recv, z_send, z_recv,
):
    s, d = lax.axis_index("sp"), lax.axis_index("dp")
    chips = n_dp // 2
    chip, core = d // 2, d % 2
    partner = d + 1 - 2 * core
    peers = chip_peers(chip, chips)
    relay = chips == 4
    tok = x.shape[0]
    heads = sh_all.shape[1]
    parts = kv.shape[0]
    groups = parts // 2
    per_group = heads // groups

    loads = []
    for part in range(parts):
        source = (wk_hbm, wv_hbm)[part // groups].at[:, pl.ds(part % groups * HEAD_DIM, HEAD_DIM)]
        loads.append(pltpu.make_async_copy(source, w_all.at[part, d], load_sem.at[part]))
    load_sh = pltpu.make_async_copy(sh_hbm, sh_all.at[s], load_sem.at[parts])
    load_x = pltpu.make_async_copy(x_hbm, x, load_sem.at[parts + 1])
    load_q = pltpu.make_async_copy(q_hbm, q, load_sem.at[parts + 2])
    for load in loads + [load_sh, load_x, load_q]:
        load.start()

    barrier = pltpu.get_barrier_semaphore()
    for to, _ in peers:
        pl.semaphore_signal(barrier, inc=1, device_id={"dp": to * 2 + core}, device_id_type=MESH)
    pl.semaphore_signal(barrier, inc=1, device_id={"dp": partner}, device_id_type=MESH)
    for t in range(1, n_sp):
        pl.semaphore_signal(barrier, inc=1, device_id={"sp": (s + t) % n_sp}, device_id_type=MESH)
    row = lax.broadcasted_iota(jnp.int32, tri.shape, 0)
    col = lax.broadcasted_iota(jnp.int32, tri.shape, 1)
    tri[...] = ((row > col) | (col >= tok)).astype(jnp.bfloat16)
    pl.semaphore_wait(barrier, chips - 1 + 1 + n_sp - 1)

    def ici_copy(part, k, block, to):
        return pltpu.make_async_remote_copy(
            src_ref=w_all.at[part, block], dst_ref=w_all.at[part, block],
            send_sem=ici_send.at[part, k], recv_sem=ici_recv.at[part, k],
            device_id={"dp": to * 2 + core}, device_id_type=MESH)

    def d2d_copy(part, k, block):
        return pltpu.make_async_remote_copy(
            src_ref=w_all.at[part, block], dst_ref=w_all.at[part, block],
            send_sem=d2d_send.at[part, k], recv_sem=d2d_recv.at[part, k],
            device_id={"dp": partner}, device_id_type=MESH)

    def z_copy(part, t, block, to):
        ref = sh_all.at[block] if part == parts else kv.at[part, block]
        return pltpu.make_async_remote_copy(
            src_ref=ref, dst_ref=ref,
            send_sem=z_send.at[part, t], recv_sem=z_recv.at[part, t],
            device_id={"sp": to}, device_id_type=MESH)

    def send_up(part):
        for t in range(1, n_sp):
            @pl.when(s + t < n_sp)
            def _(t=t):
                z_copy(part, t, s, s + t).start()

    def send_own(part):
        loads[part].wait()
        for k, (to, _) in enumerate(peers, 1):
            if not (relay and k == 3):
                ici_copy(part, k, d, to).start()
        d2d_copy(part, 0, d).start()

    def arrive(part, k):
        block = peers[k - 1][1] * 2 + core
        ici_copy(part, k, block, chip).wait_recv()
        d2d_copy(part, k, block).start()
        if relay and k < 3:
            @pl.when(core == k - 1)
            def _():
                ici_copy(part, 3, block, peers[2 - k][0]).start()

    def near(part):
        if relay:
            arrive(part, 1)
            arrive(part, 2)

    def finish(part):
        for k in range(3 if relay else 1, chips):
            arrive(part, k)
        d2d_copy(part, 0, partner).wait_recv()
        for k, (_, source) in enumerate(peers, 1):
            d2d_copy(part, k, source * 2 + 1 - core).wait_recv()
        weight = w_all[part].reshape(x.shape[1], HEAD_DIM)
        kv[part, s] = jnp.dot(x[...], weight, preferred_element_type=jnp.float32).astype(jnp.bfloat16)
        send_up(part)

    def weigh(block, diagonal):
        shift = sh_all[block].astype(jnp.float32) * LOG2E
        scale = HEAD_DIM ** -0.5 * LOG2E
        if diagonal:
            visible = lax.broadcasted_iota(jnp.int32, (tok, tok), 1) < lax.broadcasted_iota(
                jnp.int32, (tok, tok), 0)
        for h in range(heads):
            g = h // per_group
            z = lax.dot_general(
                q[:, h * HEAD_DIM:(h + 1) * HEAD_DIM], kv[g, block], NT,
                preferred_element_type=jnp.float32)
            z = z * scale + shift[h:h + 1, :]
            p = jnp.maximum(z, jnp.log(1.0 + jnp.exp2(jnp.minimum(z, 100.0))) * LOG2E)
            if diagonal:
                p = jnp.where(visible, p, 0.0)
            sums = jnp.dot(p.astype(jnp.bfloat16), tri[...], preferred_element_type=jnp.float32)
            power = z - p - sums[:, :tok]
            total = sums[:, tok:]
            if diagonal:
                w = jnp.where(visible, jnp.exp2(power), 0.0)
                carried[h] = total
            else:
                before = carried[h]
                w = jnp.exp2(power - before)
                carried[h] = before + total
            wts[block, h] = w.astype(jnp.bfloat16)

    def mix(g, block, first):
        span = slice(g * per_group, (g + 1) * per_group)
        w = wts[block, span].reshape(per_group * tok, tok)
        term = jnp.dot(w, kv[groups + g, block], preferred_element_type=jnp.float32)
        term = term.reshape(per_group, tok, HEAD_DIM)
        acc[span] = term if first else acc[span] + term

    send_own(0)
    send_own(1)
    load_sh.wait()
    send_up(parts)
    load_x.wait()
    for part in range(parts):
        near(part)
        if part + 2 < parts:
            send_own(part + 2)
        if part == parts - 1:
            load_q.wait()
            weigh(s, True)
        if part > 0:
            finish(part - 1)
    finish(parts - 1)

    @pl.loop(1, s + 1)
    def _(t):
        z_copy(parts, t, s - t, s).wait_recv()
        for g in range(groups):
            z_copy(g, t, s - t, s).wait_recv()
        weigh(s - t, False)

    for g in range(groups):
        mix(g, s, True)

    for g in range(groups):
        @pl.loop(1, s + 1)
        def _(t, g=g):
            z_copy(groups + g, t, s - t, s).wait_recv()
            mix(g, s - t, False)

    for h in range(heads):
        out_ref[:, h * HEAD_DIM:(h + 1) * HEAD_DIM] = acc[h].astype(out_ref.dtype)

    for part in range(parts):
        d2d_copy(part, 0, d).wait_send()
        for k, (to, source) in enumerate(peers, 1):
            ici_copy(part, k, d, to).wait_send()
            d2d_copy(part, k, source * 2 + core).wait_send()
    for part in range(parts + 1):
        for t in range(1, n_sp):
            @pl.when(s + t < n_sp)
            def _(part=part, t=t):
                z_copy(part, t, s, s + t).wait_send()


def per_device(n_sp, n_dp, hidden_states, queries, key_shift, key_weight, value_weight):
    seq_local, tok, model = hidden_states.shape
    assert seq_local == 1
    width, heads = queries.shape[2], key_shift.shape[2]
    rows, kv_width = key_weight.shape
    chips, parts = n_dp // 2, 2 * (kv_width // HEAD_DIM)
    bf16, f32 = jnp.bfloat16, jnp.float32
    dma = pltpu.SemaphoreType.DMA
    out = pl.pallas_call(
        functools.partial(kernel, n_sp, n_dp),
        out_shape=jax.ShapeDtypeStruct((tok, width), bf16),
        in_specs=[pl.BlockSpec(memory_space=pl.ANY)] * 5,
        out_specs=pl.BlockSpec(memory_space=pltpu.VMEM),
        scratch_shapes=[
            pltpu.VMEM((tok, model), bf16),
            pltpu.VMEM((tok, width), bf16),
            pltpu.VMEM((parts, n_dp, rows, HEAD_DIM), bf16),
            pltpu.VMEM((parts, n_sp, tok, HEAD_DIM), bf16),
            pltpu.VMEM((n_sp, heads, tok), bf16),
            pltpu.VMEM((n_sp, heads, tok, tok), bf16),
            pltpu.VMEM((heads, tok, HEAD_DIM), f32),
            pltpu.VMEM((heads, tok, tok), f32),
            pltpu.VMEM((tok, 2 * tok), bf16),
            dma((parts + 3,)),
            dma((parts, chips)), dma((parts, chips)),
            dma((parts, chips)), dma((parts, chips)),
            dma((parts + 1, n_sp)), dma((parts + 1, n_sp)),
        ],
        compiler_params=pltpu.CompilerParams(collective_id=0, has_side_effects=True),
        name="stick_breaking",
    )(hidden_states[0], queries[0], jnp.swapaxes(key_shift, 1, 2)[0], key_weight, value_weight)
    return out[None]


def solution(mesh):
    placed = (
        P("dp", "sp", None),
        P("dp", "sp", None),
        P("dp", "sp", None),
        P("dp", None),
        P("dp", None),
    )
    return jax.shard_map(
        functools.partial(per_device, mesh.shape["sp"], mesh.shape["dp"]),
        mesh=mesh, in_specs=placed, out_specs=P("dp", "sp", None), check_vma=False,
    )
```

```python
import functools
import math

import jax
import jax.numpy as jnp
from jax import lax
from jax.experimental import pallas as pl
from jax.experimental.pallas import tpu as pltpu
from jax.sharding import PartitionSpec as P

HEAD_DIM = 128
LOG2E = math.log2(math.e)
MESH = pl.DeviceIdType.MESH
NT = (((1,), (1,)), ((), ()))


def chip_peers(chip, chips):
    if chips == 4:
        x, y = chip % 2, chip // 2
        order = [chip + 1 - 2 * x, chip + 2 - 4 * y, chips - 1 - chip]
        return [(c, c) for c in order]
    return [((chip + k) % chips, (chip + chips - k) % chips) for k in range(1, chips)]


def kernel(
    n_sp, n_dp,
    x_hbm, q_hbm, sh_hbm, wk_hbm, wv_hbm, out_ref,
    x, q, w_all, kv, sh_all, wts, acc, carried, tri, power, penalty,
    load_sem, ici_send, ici_recv, d2d_send, d2d_recv, z_send, z_recv,
):
    s, d = lax.axis_index("sp"), lax.axis_index("dp")
    chips = n_dp // 2
    chip, core = d // 2, d % 2
    partner = d + 1 - 2 * core
    peers = chip_peers(chip, chips)
    relay = chips == 4
    tok = x.shape[0]
    heads = sh_all.shape[1]
    parts = kv.shape[0]
    groups = parts // 2
    per_group = heads // groups

    loads = []
    for part in range(parts):
        source = (wk_hbm, wv_hbm)[part // groups].at[:, pl.ds(part % groups * HEAD_DIM, HEAD_DIM)]
        loads.append(pltpu.make_async_copy(source, w_all.at[part, d], load_sem.at[part]))
    load_sh = pltpu.make_async_copy(sh_hbm, sh_all.at[s], load_sem.at[parts])
    load_x = pltpu.make_async_copy(x_hbm, x, load_sem.at[parts + 1])
    load_q = pltpu.make_async_copy(q_hbm, q, load_sem.at[parts + 2])
    for load in loads + [load_sh, load_x, load_q]:
        load.start()

    barrier = pltpu.get_barrier_semaphore()
    for to, _ in peers:
        pl.semaphore_signal(barrier, inc=1, device_id={"dp": to * 2 + core}, device_id_type=MESH)
    pl.semaphore_signal(barrier, inc=1, device_id={"dp": partner}, device_id_type=MESH)
    for t in range(1, n_sp):
        pl.semaphore_signal(barrier, inc=1, device_id={"sp": (s + t) % n_sp}, device_id_type=MESH)
    row = lax.broadcasted_iota(jnp.int32, tri.shape, 0)
    col = lax.broadcasted_iota(jnp.int32, tri.shape, 1)
    tri[...] = ((row > col) | (col >= tok)).astype(jnp.bfloat16)
    pl.semaphore_wait(barrier, chips - 1 + 1 + n_sp - 1)

    def ici_copy(part, k, block, to):
        return pltpu.make_async_remote_copy(
            src_ref=w_all.at[part, block], dst_ref=w_all.at[part, block],
            send_sem=ici_send.at[part, k], recv_sem=ici_recv.at[part, k],
            device_id={"dp": to * 2 + core}, device_id_type=MESH)

    def d2d_copy(part, k, block):
        return pltpu.make_async_remote_copy(
            src_ref=w_all.at[part, block], dst_ref=w_all.at[part, block],
            send_sem=d2d_send.at[part, k], recv_sem=d2d_recv.at[part, k],
            device_id={"dp": partner}, device_id_type=MESH)

    def z_copy(part, t, block, to):
        ref = sh_all.at[block] if part == parts else kv.at[part, block]
        return pltpu.make_async_remote_copy(
            src_ref=ref, dst_ref=ref,
            send_sem=z_send.at[part, t], recv_sem=z_recv.at[part, t],
            device_id={"sp": to}, device_id_type=MESH)

    def send_up(part):
        for t in range(1, n_sp):
            @pl.when(s + t < n_sp)
            def _(t=t):
                z_copy(part, t, s, s + t).start()

    def send_own(part):
        loads[part].wait()
        for k, (to, _) in enumerate(peers, 1):
            if not (relay and k == 3):
                ici_copy(part, k, d, to).start()
        d2d_copy(part, 0, d).start()

    def arrive(part, k):
        block = peers[k - 1][1] * 2 + core
        ici_copy(part, k, block, chip).wait_recv()
        d2d_copy(part, k, block).start()
        if relay and k < 3:
            @pl.when(core == k - 1)
            def _():
                ici_copy(part, 3, block, peers[2 - k][0]).start()

    def near(part):
        if relay:
            arrive(part, 1)
            arrive(part, 2)

    def finish(part):
        for k in range(3 if relay else 1, chips):
            arrive(part, k)
        d2d_copy(part, 0, partner).wait_recv()
        for k, (_, source) in enumerate(peers, 1):
            d2d_copy(part, k, source * 2 + 1 - core).wait_recv()
        weight = w_all[part].reshape(x.shape[1], HEAD_DIM)
        kv[part, s] = jnp.dot(x[...], weight, preferred_element_type=jnp.float32).astype(jnp.bfloat16)
        send_up(part)

    def weigh(block, diagonal):
        shift = sh_all[block].astype(jnp.float32) * LOG2E
        scale = HEAD_DIM ** -0.5 * LOG2E
        if diagonal:
            visible = lax.broadcasted_iota(jnp.int32, (tok, tok), 1) < lax.broadcasted_iota(
                jnp.int32, (tok, tok), 0)
        def first_pass(h, g):
            z = lax.dot_general(
                q[:, h * HEAD_DIM:(h + 1) * HEAD_DIM], kv[g, block], NT, preferred_element_type=jnp.float32)
            z = z * scale + shift[h:h + 1, :]
            p = jnp.maximum(z, jnp.log(1.0 + jnp.exp2(jnp.minimum(z, 100.0))) * LOG2E)
            if diagonal:
                p = jnp.where(visible, p, 0.0)
            power[h] = z - p
            penalty[h] = p.astype(jnp.bfloat16)

        def second_pass(h):
            sums = jnp.dot(penalty[h], tri[...], preferred_element_type=jnp.float32)
            left = power[h] - sums[:, :tok]
            if diagonal:
                w = jnp.where(visible, jnp.exp2(left), 0.0)
                carried[h] = sums[:, tok:]
            else:
                before = carried[h]
                w = jnp.exp2(left - before)
                carried[h] = before + sums[:, tok:]
            wts[block, h] = w.astype(jnp.bfloat16)

        for h in range(heads):
            first_pass(h, h // per_group)
        for h in range(heads):
            second_pass(h)

    def mix(g, block, first):
        span = slice(g * per_group, (g + 1) * per_group)
        w = wts[block, span].reshape(per_group * tok, tok)
        term = jnp.dot(w, kv[groups + g, block], preferred_element_type=jnp.float32)
        term = term.reshape(per_group, tok, HEAD_DIM)
        acc[span] = term if first else acc[span] + term

    send_own(0)
    send_own(1)
    load_sh.wait()
    send_up(parts)
    load_x.wait()
    for part in range(parts):
        near(part)
        if part + 2 < parts:
            send_own(part + 2)
        if part == parts - 1:
            load_q.wait()
            weigh(s, True)
        if part > 0:
            finish(part - 1)
    finish(parts - 1)

    @pl.loop(1, s + 1)
    def _(t):
        z_copy(parts, t, s - t, s).wait_recv()
        for g in range(groups):
            z_copy(g, t, s - t, s).wait_recv()
        weigh(s - t, False)

    for g in range(groups):
        mix(g, s, True)

    for g in range(groups):
        @pl.loop(1, s + 1)
        def _(t, g=g):
            z_copy(groups + g, t, s - t, s).wait_recv()
            mix(g, s - t, False)

    for h in range(heads):
        out_ref[:, h * HEAD_DIM:(h + 1) * HEAD_DIM] = acc[h].astype(out_ref.dtype)

    for part in range(parts):
        d2d_copy(part, 0, d).wait_send()
        for k, (to, source) in enumerate(peers, 1):
            ici_copy(part, k, d, to).wait_send()
            d2d_copy(part, k, source * 2 + core).wait_send()
    for part in range(parts + 1):
        for t in range(1, n_sp):
            @pl.when(s + t < n_sp)
            def _(part=part, t=t):
                z_copy(part, t, s, s + t).wait_send()


def per_device(n_sp, n_dp, hidden_states, queries, key_shift, key_weight, value_weight):
    seq_local, tok, model = hidden_states.shape
    assert seq_local == 1
    width, heads = queries.shape[2], key_shift.shape[2]
    rows, kv_width = key_weight.shape
    chips, parts = n_dp // 2, 2 * (kv_width // HEAD_DIM)
    bf16, f32 = jnp.bfloat16, jnp.float32
    dma = pltpu.SemaphoreType.DMA
    out = pl.pallas_call(
        functools.partial(kernel, n_sp, n_dp),
        out_shape=jax.ShapeDtypeStruct((tok, width), bf16),
        in_specs=[pl.BlockSpec(memory_space=pl.ANY)] * 5,
        out_specs=pl.BlockSpec(memory_space=pltpu.VMEM),
        scratch_shapes=[
            pltpu.VMEM((tok, model), bf16),
            pltpu.VMEM((tok, width), bf16),
            pltpu.VMEM((parts, n_dp, rows, HEAD_DIM), bf16),
            pltpu.VMEM((parts, n_sp, tok, HEAD_DIM), bf16),
            pltpu.VMEM((n_sp, heads, tok), bf16),
            pltpu.VMEM((n_sp, heads, tok, tok), bf16),
            pltpu.VMEM((heads, tok, HEAD_DIM), f32),
            pltpu.VMEM((heads, tok, tok), f32),
            pltpu.VMEM((tok, 2 * tok), bf16),
            pltpu.VMEM((heads, tok, tok), f32),
            pltpu.VMEM((heads, tok, tok), bf16),
            dma((parts + 3,)),
            dma((parts, chips)), dma((parts, chips)),
            dma((parts, chips)), dma((parts, chips)),
            dma((parts + 1, n_sp)), dma((parts + 1, n_sp)),
        ],
        compiler_params=pltpu.CompilerParams(
            collective_id=0, has_side_effects=True),
        name="stick_breaking",
    )(hidden_states[0], queries[0], jnp.swapaxes(key_shift, 1, 2)[0], key_weight, value_weight)
    return out[None]


def solution(mesh):
    placed = (
        P("dp", "sp", None),
        P("dp", "sp", None),
        P("dp", "sp", None),
        P("dp", None),
        P("dp", None),
    )
    return jax.shard_map(
        functools.partial(per_device, mesh.shape["sp"], mesh.shape["dp"]),
        mesh=mesh, in_specs=placed, out_specs=P("dp", "sp", None), check_vma=False,
    )
```

```python
import functools
import math

import jax
import jax.numpy as jnp
from jax import lax
from jax.experimental import pallas as pl
from jax.experimental.pallas import tpu as pltpu
from jax.sharding import PartitionSpec as P

HEAD_DIM = 128
LOG2E = math.log2(math.e)
MESH = pl.DeviceIdType.MESH
NT = (((1,), (1,)), ((), ()))


def chip_peers(chip, chips):
    if chips == 4:
        x, y = chip % 2, chip // 2
        order = [chip + 1 - 2 * x, chip + 2 - 4 * y, chips - 1 - chip]
        return [(c, c) for c in order]
    return [((chip + k) % chips, (chip + chips - k) % chips) for k in range(1, chips)]


def kernel(
    n_sp, n_dp,
    x_hbm, q_hbm, sh_hbm, wk_hbm, wv_hbm, out_hbm,
    x, q, w_all, kv, sh_all, wts, acc, carried, tri, power, penalty, staged,
    load_sem, ici_send, ici_recv, d2d_send, d2d_recv, z_send, z_recv, out_sem,
):
    s, d = lax.axis_index("sp"), lax.axis_index("dp")
    chips = n_dp // 2
    chip, core = d // 2, d % 2
    partner = d + 1 - 2 * core
    peers = chip_peers(chip, chips)
    relay = chips == 4
    tok = x.shape[0]
    heads = sh_all.shape[1]
    parts = kv.shape[0]
    groups = parts // 2
    per_group = heads // groups

    loads = []
    for part in range(parts):
        source = (wk_hbm, wv_hbm)[part // groups].at[:, pl.ds(part % groups * HEAD_DIM, HEAD_DIM)]
        loads.append(pltpu.make_async_copy(source, w_all.at[part, d], load_sem.at[part]))
    load_sh = pltpu.make_async_copy(sh_hbm, sh_all.at[s], load_sem.at[parts])
    load_x = pltpu.make_async_copy(x_hbm, x, load_sem.at[parts + 1])
    load_q = pltpu.make_async_copy(q_hbm, q, load_sem.at[parts + 2])
    for load in loads + [load_sh, load_x, load_q]:
        load.start()

    barrier = pltpu.get_barrier_semaphore()
    for to, _ in peers:
        pl.semaphore_signal(barrier, inc=1, device_id={"dp": to * 2 + core}, device_id_type=MESH)
    pl.semaphore_signal(barrier, inc=1, device_id={"dp": partner}, device_id_type=MESH)
    for t in range(1, n_sp):
        pl.semaphore_signal(barrier, inc=1, device_id={"sp": (s + t) % n_sp}, device_id_type=MESH)
    row = lax.broadcasted_iota(jnp.int32, tri.shape, 0)
    col = lax.broadcasted_iota(jnp.int32, tri.shape, 1)
    tri[...] = ((row > col) | (col >= tok)).astype(jnp.bfloat16)
    pl.semaphore_wait(barrier, chips - 1 + 1 + n_sp - 1)

    def ici_copy(part, k, block, to):
        return pltpu.make_async_remote_copy(
            src_ref=w_all.at[part, block], dst_ref=w_all.at[part, block],
            send_sem=ici_send.at[part, k], recv_sem=ici_recv.at[part, k],
            device_id={"dp": to * 2 + core}, device_id_type=MESH)

    def d2d_copy(part, k, block):
        return pltpu.make_async_remote_copy(
            src_ref=w_all.at[part, block], dst_ref=w_all.at[part, block],
            send_sem=d2d_send.at[part, k], recv_sem=d2d_recv.at[part, k],
            device_id={"dp": partner}, device_id_type=MESH)

    def z_copy(part, t, block, to):
        ref = sh_all.at[block] if part == parts else kv.at[part, block]
        return pltpu.make_async_remote_copy(
            src_ref=ref, dst_ref=ref,
            send_sem=z_send.at[part, t], recv_sem=z_recv.at[part, t],
            device_id={"sp": to}, device_id_type=MESH)

    def send_up(part):
        for t in reversed(range(1, n_sp)):
            @pl.when(s + t < n_sp)
            def _(t=t):
                z_copy(part, t, s, s + t).start()

    def send_own(part):
        loads[part].wait()
        for k, (to, _) in enumerate(peers, 1):
            if not (relay and k == 3):
                ici_copy(part, k, d, to).start()
        d2d_copy(part, 0, d).start()

    def arrive(part, k):
        block = peers[k - 1][1] * 2 + core
        ici_copy(part, k, block, chip).wait_recv()
        d2d_copy(part, k, block).start()
        if relay and k < 3:
            @pl.when(core == k - 1)
            def _():
                ici_copy(part, 3, block, peers[2 - k][0]).start()

    def near(part):
        if relay:
            arrive(part, 1)
            arrive(part, 2)

    def finish(part):
        for k in range(3 if relay else 1, chips):
            arrive(part, k)
        d2d_copy(part, 0, partner).wait_recv()
        for k, (_, source) in enumerate(peers, 1):
            d2d_copy(part, k, source * 2 + 1 - core).wait_recv()
        weight = w_all[part].reshape(x.shape[1], HEAD_DIM)
        kv[part, s] = jnp.dot(x[...], weight, preferred_element_type=jnp.float32).astype(jnp.bfloat16)
        send_up(part)

    def weigh(block, diagonal):
        shift = sh_all[block].astype(jnp.float32) * LOG2E
        scale = HEAD_DIM ** -0.5 * LOG2E
        if diagonal:
            visible = lax.broadcasted_iota(jnp.int32, (tok, tok), 1) < lax.broadcasted_iota(
                jnp.int32, (tok, tok), 0)
        def first_pass(h, g):
            z = lax.dot_general(
                q[:, h * HEAD_DIM:(h + 1) * HEAD_DIM], kv[g, block], NT, preferred_element_type=jnp.float32)
            z = z * scale + shift[h:h + 1, :]
            p = jnp.maximum(z, jnp.log(1.0 + jnp.exp2(jnp.minimum(z, 100.0))) * LOG2E)
            if diagonal:
                p = jnp.where(visible, p, 0.0)
            power[h] = z - p
            penalty[h] = p.astype(jnp.bfloat16)

        def second_pass(h):
            sums = jnp.dot(penalty[h], tri[...], preferred_element_type=jnp.float32)
            left = power[h] - sums[:, :tok]
            if diagonal:
                w = jnp.where(visible, jnp.exp2(left), 0.0)
                carried[h] = sums[:, tok:]
            else:
                before = carried[h]
                w = jnp.exp2(left - before)
                carried[h] = before + sums[:, tok:]
            wts[block, h] = w.astype(jnp.bfloat16)

        for h in range(heads):
            first_pass(h, h // per_group)
        for h in range(heads):
            second_pass(h)

    def mix(g, block, first):
        span = slice(g * per_group, (g + 1) * per_group)
        w = wts[block, span].reshape(per_group * tok, tok)
        term = jnp.dot(w, kv[groups + g, block], preferred_element_type=jnp.float32)
        term = term.reshape(per_group, tok, HEAD_DIM)
        acc[span] = term if first else acc[span] + term

    send_own(0)
    send_own(1)
    load_sh.wait()
    send_up(parts)
    load_x.wait()
    for part in range(parts):
        near(part)
        if part + 2 < parts:
            send_own(part + 2)
        if part == parts - 1:
            load_q.wait()
            weigh(s, True)
        if part > 0:
            finish(part - 1)
    finish(parts - 1)

    @pl.loop(1, s + 1)
    def _(t):
        z_copy(parts, t, s - t, s).wait_recv()
        for g in range(groups):
            z_copy(g, t, s - t, s).wait_recv()
        weigh(s - t, False)

    for g in range(groups):
        mix(g, s, True)

    def store(g):
        columns = pl.ds(g * per_group * HEAD_DIM, per_group * HEAD_DIM)
        return pltpu.make_async_copy(staged.at[:, columns], out_hbm.at[:, columns], out_sem.at[g])

    for g in range(groups):
        @pl.loop(1, s + 1)
        def _(t, g=g):
            z_copy(groups + g, t, s - t, s).wait_recv()
            mix(g, s - t, False)

        for h in range(g * per_group, (g + 1) * per_group):
            staged[:, h * HEAD_DIM:(h + 1) * HEAD_DIM] = acc[h].astype(staged.dtype)
        store(g).start()

    for part in range(parts):
        d2d_copy(part, 0, d).wait_send()
        for k, (to, source) in enumerate(peers, 1):
            ici_copy(part, k, d, to).wait_send()
            d2d_copy(part, k, source * 2 + core).wait_send()
    for part in range(parts + 1):
        for t in range(1, n_sp):
            @pl.when(s + t < n_sp)
            def _(part=part, t=t):
                z_copy(part, t, s, s + t).wait_send()
    for g in range(groups):
        store(g).wait()


def per_device(n_sp, n_dp, hidden_states, queries, key_shift, key_weight, value_weight):
    seq_local, tok, model = hidden_states.shape
    assert seq_local == 1
    width, heads = queries.shape[2], key_shift.shape[2]
    rows, kv_width = key_weight.shape
    chips, parts = n_dp // 2, 2 * (kv_width // HEAD_DIM)
    bf16, f32 = jnp.bfloat16, jnp.float32
    dma = pltpu.SemaphoreType.DMA
    out = pl.pallas_call(
        functools.partial(kernel, n_sp, n_dp),
        out_shape=jax.ShapeDtypeStruct((tok, width), bf16),
        in_specs=[pl.BlockSpec(memory_space=pl.ANY)] * 5,
        out_specs=pl.BlockSpec(memory_space=pl.ANY),
        scratch_shapes=[
            pltpu.VMEM((tok, model), bf16),
            pltpu.VMEM((tok, width), bf16),
            pltpu.VMEM((parts, n_dp, rows, HEAD_DIM), bf16),
            pltpu.VMEM((parts, n_sp, tok, HEAD_DIM), bf16),
            pltpu.VMEM((n_sp, heads, tok), bf16),
            pltpu.VMEM((n_sp, heads, tok, tok), bf16),
            pltpu.VMEM((heads, tok, HEAD_DIM), f32),
            pltpu.VMEM((heads, tok, tok), f32),
            pltpu.VMEM((tok, 2 * tok), bf16),
            pltpu.VMEM((heads, tok, tok), f32),
            pltpu.VMEM((heads, tok, tok), bf16),
            pltpu.VMEM((tok, width), bf16),
            dma((parts + 3,)),
            dma((parts, chips)), dma((parts, chips)),
            dma((parts, chips)), dma((parts, chips)),
            dma((parts + 1, n_sp)), dma((parts + 1, n_sp)),
            dma((parts // 2,)),
        ],
        compiler_params=pltpu.CompilerParams(
            collective_id=0, has_side_effects=True),
        name="stick_breaking",
    )(hidden_states[0], queries[0], jnp.swapaxes(key_shift, 1, 2)[0], key_weight, value_weight)
    return out[None]


def solution(mesh):
    placed = (
        P("dp", "sp", None),
        P("dp", "sp", None),
        P("dp", "sp", None),
        P("dp", None),
        P("dp", None),
    )
    return jax.shard_map(
        functools.partial(per_device, mesh.shape["sp"], mesh.shape["dp"]),
        mesh=mesh, in_specs=placed, out_specs=P("dp", "sp", None), check_vma=False,
    )
```
